32 devices in a mesh: ep: 32 (over z, y, x, core).
Axes of the slice: x: 2, y: 2, z: 4, core: 2. Of those that a mesh axis runs over, the one named last changes fastest.
Arguments:
- residual: bfloat16 [2048, 2048], P('ep'), may hold values from -6 to 6
- branch_in: bfloat16 [2048, 1024], P('ep'), may hold values from -6 to 6
- state_real: float32 [2048, 4096], P('ep'), may hold values from -4 to 4
- state_imag: float32 [2048, 4096], P('ep'), may hold values from -4 to 4
- decay_rate: float32 [64, 64], replicated, may hold values from 0.1 to 1
- frequency: float32 [64, 64], replicated, may hold values from 0 to 200
- log_step: float32 [64], replicated, may hold values from -4 to 0
- input_real: bfloat16 [64, 64, 16], replicated, may hold values from -1 to 1
- input_imag: bfloat16 [64, 64, 16], replicated, may hold values from -1 to 1
- output_matrix_real: bfloat16 [64, 16, 64], replicated, may hold values from -0.5 to 0.5
- output_matrix_imaginary: bfloat16 [64, 16, 64], replicated, may hold values from -0.5 to 0.5
- skip_gain: float32 [1024], replicated, may hold values from -4 to 4
- glu_value: bfloat16 [1024, 2048], replicated, may hold values from -0.1875 to 0.1875
- glu_gate: bfloat16 [1024, 2048], replicated, may hold values from -0.1875 to 0.1875
- mix_gain: float32 [2048], replicated, may hold values from 0.1 to 1.9
- moe_in_gain: float32 [2048], replicated, may hold values from 0.1 to 1.9
- moe_out_gain: float32 [2048], replicated, may hold values from 0.1 to 1.9
- routes: int32 [2048, 6], P('ep'), may hold values from 0 to 31, all different within a row; in each aligned block of 64 rows (0 to 63, 64 to 127, ...) at most 16 rows name the same one
- route_weights: float32 [2048, 6], P('ep'), may hold values from 0.05 to 0.6
- expert_gate: bfloat16 [32, 2048, 512], P('ep'), may hold values from -0.125 to 0.125
- expert_up: bfloat16 [32, 2048, 512], P('ep'), may hold values from -0.125 to 0.125
- expert_down: bfloat16 [32, 512, 2048], P('ep'), may hold values from -0.25 to 0.25
- shared_gate: bfloat16 [2048, 512], replicated, may hold values from -0.125 to 0.125
- shared_up: bfloat16 [2048, 512], replicated, may hold values from -0.125 to 0.125
- shared_down: bfloat16 [512, 2048], replicated, may hold values from -0.25 to 0.25
Outputs:
- layer_out: bfloat16 [2048, 2048], P('ep')
- next_real: float32 [2048, 4096], P('ep')
- next_imag: float32 [2048, 4096], P('ep')
The draws below stay inside these ranges and needn't reach their ends.
Inputs may be any that keep to these rules, and one draw needn't show every extreme that they name: `routes`: among the rows of one device no expert is named more than 16 times, and in every draw some expert is named exactly 16 times by some device's rows; a token's experts are distinct.
All inputs are finite; a program needn't handle non-finite values.
Results may differ from the reference program's by a relative error of at most 0.0066.
Values may be sent and summed in bfloat16 or wider, within the bound.
A program may use at most 128 MiB of HBM per device.

```python
import math
import jax
import jax.numpy as jnp
import numpy as np
from jax import lax

D = 2048
SSM_W = 1024
GCH = 16
GROUPS = 64
STATE = 64
EH = 512
TOP_K = 6
SEQ_DEV = 64
SEQS = 2048
EXPERTS = 32
CAP = 16
N_EP = 32


def levels(key, shape, pieces, least, largest):
    def one(dim, shards_of):
        steps = jax.random.uniform(jax.random.fold_in(jax.random.fold_in(key, 6), dim), (shards_of,), jnp.float32, least / len(pieces), largest / len(pieces))
        return jnp.repeat(jnp.exp(steps), shape[dim] // shards_of).reshape((-1,) + (1,) * (len(shape) - dim - 1))

    factor_of = one(*pieces[0])
    for cut in pieces[1:]:
        factor_of = factor_of * one(*cut)
    return factor_of


def shared_out(key, own, number, rows, amount, top, most, lean):
    ranking = jax.random.permutation(key, amount)
    heavy_load, ordinary = portions_of(amount, rows * top, most, lean, True), portions_of(amount, rows * top, most, lean, False)
    places = jnp.arange(amount)

    def named(sizes, rotation):
        used = int((sizes > 0).sum())
        fixed = max(1, used // 4)
        moved = fixed + (places - fixed + rotation * (used - fixed)) % max(1, amount - fixed)
        return jnp.zeros((amount,), jnp.int32).at[ranking[jnp.where(places < fixed, places, moved)]].set(jnp.asarray(sizes, jnp.int32))

    sizes = jnp.where(number % 4 == 0, named(heavy_load, number // 4), named(ordinary, number - number // 4 - 1))
    mixed = jax.random.permutation(jax.random.fold_in(own, 3), amount)
    source_of, sink = mixed[0:amount // 2 * 2:2], mixed[1:amount // 2 * 2:2]
    slack = jnp.minimum(sizes[source_of] - 1, most - sizes[sink]) // 2
    slack = jnp.where((source_of == ranking[0]) | (sink == ranking[0]) | (sizes[sink] == 0), 0, jnp.maximum(slack, 0))
    moved = jax.random.randint(jax.random.fold_in(own, 4), (amount // 2,), 0, 1 << 20) % (slack + 1)
    sizes = sizes.at[source_of].add(-moved).at[sink].add(moved)
    items = jnp.searchsorted(jnp.cumsum(sizes), jnp.arange(rows * top), side="right").astype(jnp.int32)
    table = items.reshape(top, rows).T
    table = table[jax.random.permutation(jax.random.fold_in(own, 1), rows)]
    rotation = jax.random.randint(jax.random.fold_in(own, 2), (rows, 1), 0, top)
    return jnp.take_along_axis(table, (jnp.arange(top)[None, :] + rotation) % top, axis=1)


def portions_of(amount, total, reach, skew, full):
    weights = [(1 << 20) // math.isqrt(rank ** skew) + 1 for rank in range(1, amount + 1)]
    largest = reach if full else min(reach, max(-(-total // amount), total * weights[0] // sum(weights)))
    least = 1 if total - largest >= amount - 1 else 0
    given, surplus = [largest] + [least] * (amount - 1), total - largest - least * (amount - 1)
    while surplus > 0:
        candidates = [i for i in range(1, amount) if given[i] < largest] or [i for i in range(1, amount) if given[i] < reach]
        whole, left = sum([weights[i] for i in candidates]), surplus
        for i in candidates:
            more = min(reach - given[i], max(1, left * weights[i] // whole), surplus)
            given[i] = given[i] + more
            surplus = surplus - more
    return np.array(given)


def bell_draw(rng, shape, deviation, reach, split=(), kind=jnp.bfloat16):
    loudness = levels(rng, shape, split, -0.22, 0.18) if split else 1.0
    array = jax.random.normal(rng, shape, jnp.float32) * deviation * loudness
    return jnp.minimum(jnp.maximum(array, -reach), reach).astype(kind)


def setup_inputs(seed: int = 0) -> dict:
    arg_keys = jax.random.split(jax.random.key(seed), 26)
    residual = bell_draw(arg_keys[0], (SEQS, D), 1.0, 6.0, ((0, 32),))
    branch_in = bell_draw(arg_keys[1], (SEQS, SSM_W), 1.0, 6.0, ((0, 32),))
    state_real = bell_draw(arg_keys[2], (SEQS, GROUPS * STATE), 0.5, 4.0, ((0, 32),), jnp.float32)
    state_imag = bell_draw(arg_keys[3], (SEQS, GROUPS * STATE), 0.5, 4.0, ((0, 32),), jnp.float32)
    decay_rate = jnp.clip(jnp.exp(jax.random.uniform(arg_keys[4], (GROUPS, STATE), jnp.float32, math.log(0.1), math.log(1.0))), 0.1, 1.0)
    frequency = jnp.clip(jax.random.uniform(arg_keys[5], (GROUPS, STATE), jnp.float32, 0.0, 200.0), 0.0, 200.0)
    log_step = jnp.clip(jax.random.uniform(arg_keys[6], (GROUPS,), jnp.float32, -4.0, 0.0), -4.0, 0.0)
    input_real = bell_draw(arg_keys[7], (GROUPS, STATE, GCH), (2 * GCH) ** -0.5, 1.0)
    input_imag = bell_draw(arg_keys[8], (GROUPS, STATE, GCH), (2 * GCH) ** -0.5, 1.0)
    output_matrix_real = bell_draw(arg_keys[9], (GROUPS, GCH, STATE), (2 * STATE) ** -0.5, 0.5)
    output_matrix_imaginary = bell_draw(arg_keys[10], (GROUPS, GCH, STATE), (2 * STATE) ** -0.5, 0.5)
    skip_gain = bell_draw(arg_keys[11], (SSM_W,), 1.0, 4.0, (), jnp.float32)
    glu_value = bell_draw(arg_keys[12], (SSM_W, D), SSM_W ** -0.5, 0.1875)
    glu_gate = bell_draw(arg_keys[13], (SSM_W, D), SSM_W ** -0.5, 0.1875)
    mix_gain = jnp.clip(1.0 + 0.18 * jax.random.normal(arg_keys[14], (D,), jnp.float32), 0.1, 1.9)
    moe_in_gain = jnp.clip(1.0 + 0.18 * jax.random.normal(arg_keys[15], (D,), jnp.float32), 0.1, 1.9)
    moe_out_gain = jnp.clip(1.0 + 0.18 * jax.random.normal(arg_keys[16], (D,), jnp.float32), 0.1, 1.9)
    routes_keys = jax.random.split(jax.random.fold_in(arg_keys[17], 1), SEQS // SEQ_DEV)
    routes_turns = jax.random.permutation(jax.random.fold_in(arg_keys[17], 3), SEQS // SEQ_DEV)
    routes = jax.vmap(lambda own, number: shared_out(jax.random.fold_in(arg_keys[17], 2), own, number, SEQ_DEV, EXPERTS, TOP_K, CAP, 2))(routes_keys, routes_turns).reshape((SEQS, TOP_K))
    route_weights = jnp.clip(0.05 + 0.55 * jax.random.uniform(arg_keys[18], (SEQS, TOP_K), jnp.float32) ** levels(arg_keys[18], (SEQS, TOP_K), ((0, 32),), -0.2, 0.2), 0.05, 0.6)
    expert_gate = bell_draw(arg_keys[19], (EXPERTS, D, EH), D ** -0.5, 0.125, ((0, 32),))
    expert_up = bell_draw(arg_keys[20], (EXPERTS, D, EH), D ** -0.5, 0.125, ((0, 32),))
    expert_down = bell_draw(arg_keys[21], (EXPERTS, EH, D), EH ** -0.5, 0.25, ((0, 32),))
    shared_gate = bell_draw(arg_keys[22], (D, EH), D ** -0.5, 0.125)
    shared_up = bell_draw(arg_keys[23], (D, EH), D ** -0.5, 0.125)
    shared_down = bell_draw(arg_keys[24], (EH, D), EH ** -0.5, 0.25)
    return dict(residual=residual, branch_in=branch_in, state_real=state_real, state_imag=state_imag, decay_rate=decay_rate, frequency=frequency, log_step=log_step, input_real=input_real, input_imag=input_imag, output_matrix_real=output_matrix_real, output_matrix_imaginary=output_matrix_imaginary, skip_gain=skip_gain, glu_value=glu_value, glu_gate=glu_gate, mix_gain=mix_gain, moe_in_gain=moe_in_gain, moe_out_gain=moe_out_gain, routes=routes, route_weights=route_weights, expert_gate=expert_gate, expert_up=expert_up, expert_down=expert_down, shared_gate=shared_gate, shared_up=shared_up, shared_down=shared_down)


norm_eps = 1e-06

def scaled_norm(row_block, norm_gain):
    return row_block * lax.rsqrt(lax.optimization_barrier(jnp.mean(row_block * row_block, axis=-1, keepdims=True)) + norm_eps) * norm_gain

def state_step(branch_in, state_real, state_imag, decay_rate, frequency, log_step, input_real, input_imag, output_matrix_real, output_matrix_imaginary, skip_gain):
    seq_count = branch_in.shape[0]
    group_count, state_count = decay_rate.shape
    chan_count = input_real.shape[2]
    step_size = jnp.exp(log_step)[:, None]
    magnitude = jnp.exp(-decay_rate * step_size)
    abar_re = magnitude * jnp.cos(frequency * step_size)
    abar_im = magnitude * jnp.sin(frequency * step_size)
    lam_re = -decay_rate
    lam_im = frequency
    denominator = lam_re * lam_re + lam_im * lam_im
    numer_re = abar_re - 1.0
    coef_re = (numer_re * lam_re + abar_im * lam_im) / denominator
    coef_im = (abar_im * lam_re - numer_re * lam_im) / denominator
    b_real = input_real.astype(jnp.float32)
    b_imag = input_imag.astype(jnp.float32)
    bbar_re = coef_re[..., None] * b_real - coef_im[..., None] * b_imag
    bbar_im = coef_re[..., None] * b_imag + coef_im[..., None] * b_real
    feed_rows = branch_in.astype(jnp.float32).reshape(seq_count, group_count, chan_count)
    forcing_real = jnp.einsum('tgc,gpc->tgp', feed_rows, bbar_re, precision=lax.Precision.HIGHEST)
    drive_im = jnp.einsum('tgc,gpc->tgp', feed_rows, bbar_im, precision=lax.Precision.HIGHEST)
    old_re = state_real.reshape(seq_count, group_count, state_count)
    old_im = state_imag.reshape(seq_count, group_count, state_count)
    fresh_real = abar_re * old_re - abar_im * old_im + forcing_real
    fresh_imaginary = abar_re * old_im + abar_im * old_re + drive_im
    state_readout = jnp.einsum('ukb,krb->ukr', fresh_real, output_matrix_real.astype(jnp.float32), precision=lax.Precision.HIGHEST) - jnp.einsum('ukb,krb->ukr', fresh_imaginary, output_matrix_imaginary.astype(jnp.float32), precision=lax.Precision.HIGHEST)
    mixed_rows = state_readout.reshape(seq_count, group_count * chan_count) + skip_gain * branch_in.astype(jnp.float32)
    activated = jax.nn.gelu(mixed_rows).astype(jnp.bfloat16)
    return (activated, fresh_real.reshape(seq_count, -1), fresh_imaginary.reshape(seq_count, -1))

def expert_rows(row_block, w_gate, w_up, w_down):
    gate_part = jnp.dot(row_block, w_gate, preferred_element_type=jnp.float32)
    up_part = jnp.dot(row_block, w_up, preferred_element_type=jnp.float32)
    hidden = (jax.nn.silu(gate_part) * up_part).astype(jnp.bfloat16)
    return jnp.dot(hidden, w_down, preferred_element_type=jnp.float32)

def mixer_residual(residual, activated, glu_value, glu_gate, mix_gain):
    value_part = jnp.dot(activated, glu_value, preferred_element_type=jnp.float32)
    gate_part = jnp.dot(activated, glu_gate, preferred_element_type=jnp.float32)
    branch = value_part * jax.nn.sigmoid(gate_part)
    return (residual.astype(jnp.float32) + scaled_norm(branch, mix_gain)).astype(jnp.bfloat16)

def reference(residual, branch_in, state_real, state_imag, decay_rate, frequency, log_step, input_real, input_imag, output_matrix_real, output_matrix_imaginary, skip_gain, glu_value, glu_gate, mix_gain, moe_in_gain, moe_out_gain, routes, route_weights, expert_gate, expert_up, expert_down, shared_gate, shared_up, shared_down):
    activated, next_real, next_imag = state_step(branch_in, state_real, state_imag, decay_rate, frequency, log_step, input_real, input_imag, output_matrix_real, output_matrix_imaginary, skip_gain)
    resid_mid = mixer_residual(residual, activated, glu_value, glu_gate, mix_gain)
    normed = scaled_norm(resid_mid.astype(jnp.float32), moe_in_gain).astype(jnp.bfloat16)
    hidden_width = normed.shape[1]
    flat_routes = routes.reshape(-1).astype(jnp.int32)
    assign_count = flat_routes.shape[0]
    sorted_order = jnp.argsort(flat_routes, stable=True).astype(jnp.int32)
    sorted_expert = flat_routes[sorted_order]
    expert_load = lax.optimization_barrier(jnp.sum((flat_routes[:, None] == jnp.arange(EXPERTS, dtype=jnp.int32)[None, :]).astype(jnp.int32), axis=0))
    load_start = jnp.cumsum(expert_load) - expert_load
    slot_rank = jnp.arange(assign_count, dtype=jnp.int32) - load_start[sorted_expert]
    slot_most = CAP * N_EP
    slot_index = (sorted_expert * slot_most + slot_rank).astype(jnp.int32)
    slot_table = jnp.full((EXPERTS * slot_most,), SEQS, jnp.int32).at[slot_index].set(sorted_order // TOP_K)
    padded = jnp.concatenate([normed, jnp.zeros((1, hidden_width), jnp.bfloat16)], axis=0)

    def one_expert(expert_args):
        row_ids, w_gate, w_up, w_down = expert_args
        return expert_rows(padded[row_ids], w_gate, w_up, w_down).astype(jnp.bfloat16)
    expert_out = lax.map(one_expert, (slot_table.reshape(EXPERTS, slot_most), expert_gate, expert_up, expert_down))
    assign_slot = jnp.zeros((assign_count,), jnp.int32).at[sorted_order].set(slot_index)
    per_assign = expert_out.reshape(-1, hidden_width)[assign_slot].reshape(SEQS, TOP_K, hidden_width).astype(jnp.float32)
    routed = lax.optimization_barrier(jnp.sum(per_assign * route_weights[..., None], axis=1))
    shared = expert_rows(normed, shared_gate, shared_up, shared_down)
    combined = shared + routed
    layer_out = (resid_mid.astype(jnp.float32) + scaled_norm(combined, moe_out_gain)).astype(jnp.bfloat16)
    return (layer_out, next_real, next_imag)
```

```python
import functools
import math

import jax
import jax.numpy as jnp
from jax import lax
from jax.experimental import pallas as pl
from jax.experimental.pallas import tpu as pltpu
from jax.sharding import PartitionSpec as P

norm_eps = 1e-06
ROW_TILE = 16
PIECES = 2
STRIPS = 4
WINDOW = 2
AHEAD = 3
LAG = 1
VMEM_MOST = 60 * 1024 * 1024
SPARE = 8 * 1024 * 1024
MESH = pl.DeviceIdType.MESH


def scaled_norm(row_block, norm_gain):
    return (
        row_block
        * lax.rsqrt(jnp.mean(row_block * row_block, axis=-1, keepdims=True) + norm_eps)
        * norm_gain
    )


def in_hbm(*arrays):
    return [pltpu.with_memory_space_constraint(array, pltpu.HBM) for array in arrays]


def flipped(index, mask):
    out, bit = 0, 1
    while bit <= mask or bit == 1:
        digit = (index // bit) % 2
        out = out + bit * ((digit + 1) % 2 if mask & bit else digit)
        bit *= 2
    return out + (index // bit) * bit


def pick_from(table, z, k):
    value, planes = 0, len(table)
    for row in range(planes):
        away = ((z - row + planes) % planes + planes - 1) // planes
        value = value + table[row][k] * (1 - away)
    return value


def block_order(planes):
    half = max(1, planes // 2)
    order = []
    for z in range(planes):
        others = [b for b in range(planes) if b != z]
        order.append([z] + sorted(others, key=lambda b: (b // half != z // half, abs(b - z), b)))
    return order


def moe_kernel(
    planes,
    width,
    cap,
    top,
    normed,
    resid,
    out_gain_hbm,
    eg_hbm,
    eu_hbm,
    ed_hbm,
    sg_hbm,
    su_hbm,
    sd_hbm,
    out,
    eg,
    eu,
    ed,
    sg,
    su,
    sd,
    out_gain,
    col_rows,
    mix,
    x_send,
    x_recv,
    y_send,
    y_recv,
    part,
    p_send,
    q_recv,
    total,
    load_sem,
    z_s,
    row_r,
    x_s,
    x_r,
    y_s,
    y_r,
    p_s,
    q_r,
):
    me = lax.axis_index("ep")
    z = me // width
    p = me % width
    seq, model = resid.shape
    head = normed.shape[1] - model
    pad = -(-top // 8) * 8
    slots = width * cap
    chunk = model // PIECES
    columns = [slice(i * chunk, (i + 1) * chunk) for i in range(PIECES)]
    pieces = range(PIECES)
    last = planes - 1
    strip = model // STRIPS
    order = block_order(planes)
    upward = [[int(b > r) for b in order[r]] for r in range(planes)]
    behind = [[int(r > 0 if b > r else r < last) for b in order[r]] for r in range(planes)]
    block = [pick_from(order, z, k) for k in range(planes)]

    loads = [
        pltpu.make_async_copy(src, dst, load_sem.at[i])
        for i, (src, dst) in enumerate(
            (
                (sg_hbm, sg),
                (su_hbm, su),
                (sd_hbm, sd),
                (eg_hbm, eg),
                (eu_hbm, eu),
                (ed_hbm, ed),
                (out_gain_hbm, out_gain),
            )
        )
    ]
    for load in (*loads[6:], *loads[:6]):
        load.start()

    barrier = pltpu.get_barrier_semaphore()
    sides = ((z > 0, -1), (z < last, 1)) if planes > 1 else ()
    for there, step in sides:

        @pl.when(there)
        def _():
            pl.semaphore_signal(
                barrier, inc=1, device_id=((z + step) * width + p,), device_id_type=MESH
            )

    for r in range(1, width):
        pl.semaphore_signal(
            barrier, inc=1, device_id=(z * width + flipped(p, r),), device_id_type=MESH
        )

    x_ends, ends = [], []

    def send(src, dst, send_sem, recv_sem, target, kept):
        copy = pltpu.make_async_remote_copy(
            src_ref=src,
            dst_ref=dst,
            send_sem=send_sem,
            recv_sem=recv_sem,
            device_id=(target,),
            device_id_type=MESH,
        )
        copy.start()
        kept.append(copy)

    def arrive(buf, sem):
        pltpu.make_async_copy(buf, buf, sem).wait()

    def part_of(buf, k, q, i):
        return buf.at[k, pl.ds(pl.multiple_of(q * cap, cap), cap), columns[i]]

    def table(k):
        rows = normed[:, :head] if k == 0 else col_rows[block[k], :, :head]
        seen = rows.astype(jnp.float32).T
        slot = lax.broadcasted_iota(jnp.int32, (slots, seq), 0)
        expert = (z * width + slot // cap).astype(jnp.float32)
        chosen = jnp.zeros((slots, seq), jnp.float32)
        weight = jnp.zeros((slots, seq), jnp.float32)

        def line(group, j):
            return seen[group * pad + j : group * pad + j + 1, :]

        for j in range(top):
            hit = line(0, j) * 256.0 + line(1, j) == expert
            chosen = jnp.where(hit, 1.0, chosen)
            weight = jnp.where(hit, line(2, j) + line(3, j) + line(4, j), weight)
        earlier = jnp.where(
            lax.broadcasted_iota(jnp.int32, (seq, seq), 0)
            < lax.broadcasted_iota(jnp.int32, (seq, seq), 1),
            1.0,
            0.0,
        ).astype(jnp.bfloat16)
        rank = jnp.dot(chosen.astype(jnp.bfloat16), earlier, preferred_element_type=jnp.float32)
        place = (slot % cap).astype(jnp.float32)
        picks = jnp.where(rank == place, chosen, 0.0)
        spread = (picks * weight).T
        high = spread.astype(jnp.bfloat16)
        mix[k, :seq] = high
        mix[k, seq:] = (spread - high.astype(jnp.float32)).astype(jnp.bfloat16)
        return picks.astype(jnp.bfloat16)

    def gather(k, i, picks):
        span = slice(head + i * chunk, head + (i + 1) * chunk)
        rows = normed[:, span] if k == 0 else col_rows[block[k], :, span]
        x_send[k, :, columns[i]] = jnp.dot(
            picks, rows, preferred_element_type=jnp.float32
        ).astype(jnp.bfloat16)

    def exchange(src, dst, k, i, send_sems, recv_sems, kept):
        for r in range(1, width):
            q = flipped(p, r)
            send(
                part_of(src, k, q, i),
                part_of(dst, k, p, i),
                send_sems.at[k, r, i],
                recv_sems.at[k, r, i],
                z * width + q,
                kept,
            )
        mine = pl.ds(pl.multiple_of(p * cap, cap), cap)
        dst[k, mine, columns[i]] = src[k, mine, columns[i]]

    def gathered(dst, k, i, recv_sems):
        for r in range(1, width):
            arrive(part_of(dst, k, flipped(p, r), i), recv_sems.at[k, r, i])

    def z_piece(ref, j):
        return ref.at[:, slice(head + j * strip if j else 0, head + (j + 1) * strip)]

    def z_copy(s, f, j):
        source = (z - f + planes) % planes if s == 0 else (z + f) % planes
        buf = col_rows.at[source]
        return pltpu.make_async_remote_copy(
            src_ref=z_piece(buf if f else normed, j),
            dst_ref=z_piece(buf, j),
            send_sem=z_s.at[s, f, j],
            recv_sem=row_r.at[source, j],
            device_id=((z + 1 - 2 * s + planes) % planes * width + p,),
            device_id_type=MESH,
        )

    def moves(s, f):
        return [int(r >= f and r < last) if s == 0 else int(r <= last - f and r > 0) for r in range(planes)]

    def z_sent(s, f, j):
        z_copy(s, f, j).wait_send()

    def z_issue(s, f, j):
        def go():
            before = f * STRIPS + j - WINDOW
            if before >= 0:
                z_sent(s, before // STRIPS, before % STRIPS)
            z_copy(s, f, j).start()

        if any(moves(s, f)):
            pl.when(pick_from([[m] for m in moves(s, f)], z, 0) == 1)(go)

    def z_step(f, j):
        for s in range(2):
            if f:
                source = (z - f + planes) % planes if s == 0 else (z + f) % planes

                @pl.when(z >= f if s == 0 else z <= last - f)
                def _():
                    arrive(z_piece(col_rows.at[source], j), row_r.at[source, j])

            z_issue(s, f, j)

    def z_drain():
        for s in range(2):
            for f in range(planes):
                for j in range(STRIPS):
                    after = (f * STRIPS + j + WINDOW) // STRIPS
                    later = moves(s, after) if after < planes else [0] * planes
                    still = [m * (1 - n) for m, n in zip(moves(s, f), later)]
                    if any(still):
                        pl.when(pick_from([[m] for m in still], z, 0) == 1)(
                            functools.partial(z_sent, s, f, j)
                        )

    def dispatch(k, i, picks):
        gather(k, i, picks)
        exchange(x_send, x_recv, k, i, x_s, x_r, x_ends)

    def hidden(rows, w_gate, w_up):
        gate_part = jnp.dot(rows, w_gate[...], preferred_element_type=jnp.float32)
        up_part = jnp.dot(rows, w_up[...], preferred_element_type=jnp.float32)
        return (jax.nn.silu(gate_part) * up_part).astype(jnp.bfloat16)

    def expert(k):
        for i in pieces:
            gathered(x_recv, k, i, x_r)
        if k == 0:
            for load in loads[3:6]:
                load.wait()
        mid = hidden(x_recv[k], eg, eu)
        for i in pieces:
            y_send[k, :, columns[i]] = jnp.dot(
                mid, ed[:, columns[i]], preferred_element_type=jnp.float32
            ).astype(jnp.bfloat16)

    def give(k, i):
        exchange(y_send, y_recv, k, i, y_s, y_r, ends)

    def landed(k, i):
        gathered(y_recv, k, i, y_r)

    def weighed(k, i):
        both = jnp.dot(mix[k], y_recv[k, :, columns[i]], preferred_element_type=jnp.float32)
        return both[:seq] + both[seq:]

    def lane(j):
        return slice(j * strip, (j + 1) * strip)

    def strips_of(i):
        return range(i * STRIPS // PIECES, (i + 1) * STRIPS // PIECES)

    def passed_copy(k, j):
        up = pick_from(upward, z, k)
        return pltpu.make_async_remote_copy(
            src_ref=p_send.at[k, :, lane(j)],
            dst_ref=q_recv.at[1 - up, block[k], :, lane(j)],
            send_sem=p_s.at[k, j],
            recv_sem=q_r.at[1 - up, block[k], j],
            device_id=((z - 1 + 2 * up) * width + p,),
            device_id_type=MESH,
        )

    def combine(k, i):
        value = weighed(k, i)
        if k == 0:
            total[:, columns[i]] += value
            return
        part[k, :, columns[i]] = value

        @pl.when(pick_from(behind, z, k) == 0)
        def _():
            for j in strips_of(i):
                p_send[k, :, lane(j)] = part[k, :, lane(j)].astype(jnp.bfloat16)
                passed_copy(k, j).start()

    def merge(k, i):
        up = pick_from(upward, z, k)

        @pl.when(pick_from(behind, z, k) == 1)
        def _():
            for j in strips_of(i):
                landed = q_recv.at[1 - up, block[k], :, lane(j)]
                arrive(landed, q_r.at[1 - up, block[k], j])
                p_send[k, :, lane(j)] = (
                    part[k, :, lane(j)]
                    + q_recv[1 - up, block[k], :, lane(j)].astype(jnp.float32)
                ).astype(jnp.bfloat16)
                passed_copy(k, j).start()

    picks = table(0)
    for i in pieces:
        gather(0, i, picks)

    greeted = [[int(r > 0) + int(r < last)] for r in range(planes)]
    pl.semaphore_wait(barrier, width - 1 + pick_from(greeted, z, 0))
    for j in range(min(WINDOW, STRIPS)):
        z_step(0, j)
    for i in pieces:
        exchange(x_send, x_recv, 0, i, x_s, x_r, x_ends)

    for load in loads[:3]:
        load.wait()
    mid = hidden(normed[:, head:], sg, su)
    for i in pieces:
        total[:, columns[i]] = jnp.dot(
            mid, sd[:, columns[i]], preferred_element_type=jnp.float32
        )
    for j in range(min(WINDOW, STRIPS), STRIPS):
        z_step(0, j)
    for k in range(1, planes):
        for i in pieces:
            for j in strips_of(i):
                z_step(k, j)
            if i == 0:
                picks = table(k)
            dispatch(k, i, picks)
        expert(k - 1)
    turns = [(k, i) for k in (*range(last, 0, -1), 0) for i in pieces]
    if planes > 2:
        turns.remove((1, 0))
        turns.insert(0, (1, 0))
        give(1, 0)
    final_own = max((n for n, turn in enumerate(turns) if turn[0] == 1), default=-1)
    expert(last)
    for turn in turns[planes > 2 : AHEAD]:
        give(*turn)
    for copy in x_ends:
        copy.wait_send()
    done = []
    for n, turn in enumerate(turns):
        landed(*turn)
        if n + AHEAD < len(turns):
            give(*turns[n + AHEAD])
        combine(*turn)
        if turn[0] > 1:
            done.append(turn)
        if turn[0] > 1 and len(done) > LAG:
            merge(*done.pop(0))
        if n == final_own:
            for late in ((1, 0), *done, *((1, i) for i in pieces[1:])):
                merge(*late)
    for side, (there, _) in enumerate(sides):

        @pl.when(there)
        def _():
            for i in pieces:
                for j in strips_of(i):
                    arrive(q_recv.at[side, z, :, lane(j)], q_r.at[side, z, j])
                total[:, columns[i]] += q_recv[side, z, :, columns[i]].astype(jnp.float32)

    loads[6].wait()
    combined = total[...]
    out[...] = (
        resid[...].astype(jnp.float32) + scaled_norm(combined, out_gain[...])
    ).astype(out.dtype)
    for copy in ends:
        copy.wait_send()
    for k in range(1, planes):
        for j in range(STRIPS):
            passed_copy(k, j).wait_send()
    z_drain()


def moe_layer(
    normed,
    resid_mid,
    top,
    moe_out_gain,
    experts,
    shared_weights,
    planes,
    width,
    cap,
):
    seq_count, model = resid_mid.shape
    half_type = jnp.bfloat16
    vmem = pl.BlockSpec(memory_space=pltpu.VMEM)
    hbm = pl.BlockSpec(memory_space=pltpu.HBM)
    slots = (planes, width * cap, model)
    dense = (planes, seq_count, model)
    dma = pltpu.SemaphoreType.DMA
    weights = (*experts, *shared_weights)
    small = (moe_out_gain[None, :],)
    buffers = [(w.shape, w.dtype) for w in (*weights, *small)] + [
        ((planes, *normed.shape), half_type),
        ((planes, 2 * seq_count, width * cap), half_type),
        (slots, half_type),
        (slots, half_type),
        (slots, half_type),
        (slots, half_type),
        (dense, jnp.float32),
        (dense, half_type),
        ((2, *dense), half_type),
        ((seq_count, model), jnp.float32),
    ]
    used = sum(math.prod(shape) * jnp.dtype(kind).itemsize for shape, kind in buffers)
    return pl.pallas_call(
        functools.partial(moe_kernel, planes, width, cap, top),
        out_shape=jax.ShapeDtypeStruct((seq_count, model), half_type),
        in_specs=[vmem] * 2 + [hbm] * 7,
        out_specs=vmem,
        scratch_shapes=[pltpu.VMEM(shape, kind) for shape, kind in buffers]
        + [
            dma((7,)),
            dma((2, planes, STRIPS)),
            dma((planes, STRIPS)),
            *[dma((planes, width, PIECES))] * 4,
            dma((planes, STRIPS)),
            dma((2, planes, STRIPS)),
        ],
        compiler_params=pltpu.CompilerParams(
            collective_id=0,
            has_side_effects=True,
            vmem_limit_bytes=min(VMEM_MOST, used + SPARE),
        ),
        name="moe_exchange",
    )(normed, resid_mid, *in_hbm(*small, *weights))


def spread(block, groups, mask):
    return jnp.concatenate([block] * groups, axis=1) * mask


def halves(value):
    high = value.astype(jnp.bfloat16)
    return high, (value - high.astype(jnp.float32)).astype(jnp.bfloat16)


def group_mask(rows, groups, states):
    shape = (rows, groups * states)
    row = lax.broadcasted_iota(jnp.int32, shape, 0) // (rows // groups)
    column = lax.broadcasted_iota(jnp.int32, shape, 1) // states
    return jnp.where(row == column, 1.0, 0.0)


def mixer_kernel(groups, names, *refs):
    count_in = len(names) + 4
    given, rest = refs[:count_in], refs[count_in:]
    state_re, state_im, value_hbm, gate_hbm = given[len(names) :]
    resid_mid, normed, next_re, next_im = rest[:4]
    old_re, old_im, new_re, new_im, value, gate, active = rest[4:11]
    held = dict(zip(names, rest[11 : 11 + len(names)]))
    small_sem, in_sem, out_sem, glu_sem = rest[11 + len(names) :]
    small = {
        name: pltpu.make_async_copy(src, held[name], small_sem.at[i])
        for i, (name, src) in enumerate(zip(names, given))
    }
    decay, frequency, log_step = held["decay"], held["frequency"], held["log_step"]
    in_re, in_im, out_re, out_im = (held[m] for m in ("in_re", "in_im", "out_re", "out_im"))
    residual, feed, skip = held["residual"], held["feed"], held["skip"]
    mix_gain, in_gain = held["mix_gain"], held["in_gain"]
    group_count, states = decay.shape
    chans = in_re.shape[0] // group_count
    lanes = groups * states
    feeds = groups * chans
    count = group_count // groups

    def piece(n):
        return slice(n * lanes, (n + 1) * lanes)

    def read(n):
        return [
            pltpu.make_async_copy(src.at[:, piece(n)], dst.at[:, piece(n)], in_sem.at[k, n])
            for k, (src, dst) in enumerate(((state_re, old_re), (state_im, old_im)))
        ]

    def write(n):
        return [
            pltpu.make_async_copy(src.at[:, piece(n)], dst.at[:, piece(n)], out_sem.at[k, n])
            for k, (src, dst) in enumerate(((new_re, next_re), (new_im, next_im)))
        ]

    glu = [
        pltpu.make_async_copy(value_hbm, value, glu_sem.at[0]),
        pltpu.make_async_copy(gate_hbm, gate, glu_sem.at[1]),
    ]
    late = ("residual", "mix_gain", "in_gain")
    early = ("log_step", "decay", "frequency", "routes", "route_weights")
    for name in names:
        if name not in late:
            small[name].start()
    for n in range(count):
        for copy in read(n):
            copy.start()
    for copy in glu:
        copy.start()
    for name in late:
        small[name].start()

    for name in ("log_step", "decay", "frequency"):
        small[name].wait()
    square = (group_count, group_count)
    diagonal = lax.broadcasted_iota(jnp.int32, square, 0) == lax.broadcasted_iota(
        jnp.int32, square, 1
    )
    step_size = jnp.exp(
        jnp.sum(jnp.where(diagonal, log_step[...], 0.0), axis=1, keepdims=True)
    )
    rate, speed = decay[...], frequency[...]
    magnitude = jnp.exp(-rate * step_size)
    abar_re = magnitude * jnp.cos(speed * step_size)
    abar_im = magnitude * jnp.sin(speed * step_size)
    denominator = rate * rate + speed * speed
    numer_re = abar_re - 1.0
    coef_re = (abar_im * speed - numer_re * rate) / denominator
    coef_im = (-abar_im * rate - numer_re * speed) / denominator

    for name in ("routes", "route_weights"):
        small[name].wait()
    head = normed.shape[1] - resid_mid.shape[1]
    chosen, weight = held["routes"][...], held["route_weights"][...]
    top, seq = chosen.shape
    rest_of = -(-top // 8) * 8 - top
    upper, lower = halves(weight)
    lowest = weight - upper.astype(jnp.float32) - lower.astype(jnp.float32)
    parts = []
    for item in (chosen // 256, chosen % 256, upper, lower, lowest):
        parts += [item.astype(jnp.float32)] + [jnp.zeros((rest_of, seq), jnp.float32)] * (rest_of > 0)
    lines = jnp.concatenate(parts, axis=0)
    lines = jnp.concatenate([lines, jnp.zeros((head - lines.shape[0], seq), jnp.float32)], axis=0)
    normed[:, :head] = lines.T.astype(jnp.bfloat16)

    few = group_mask(groups, groups, states)
    many = group_mask(feeds, groups, states).astype(jnp.bfloat16)
    minus = -many
    nt = (((1,), (1,)), ((), ()))

    for name in names:
        if name not in late and name not in early:
            small[name].wait()
    for n in range(count):
        rows = slice(n * feeds, (n + 1) * feeds)
        some = slice(n * groups, (n + 1) * groups)
        u = feed[:, rows]

        def line(block):
            return jnp.sum(spread(block[some, :], groups, few), axis=0, keepdims=True)

        a_re, a_im, c_re, c_im = line(abar_re), line(abar_im), line(coef_re), line(coef_im)
        drive_re = jnp.dot(
            u, spread(in_re[rows, :], groups, many), preferred_element_type=jnp.float32
        )
        drive_im = jnp.dot(
            u, spread(in_im[rows, :], groups, many), preferred_element_type=jnp.float32
        )
        weights = jnp.concatenate(
            [spread(out_re[rows, :], groups, many), spread(out_im[rows, :], groups, minus)],
            axis=1,
        )
        for copy in read(n):
            copy.wait()
        was_re, was_im = old_re[:, piece(n)], old_im[:, piece(n)]
        fresh_re = a_re * was_re - a_im * was_im + (c_re * drive_re - c_im * drive_im)
        fresh_im = a_re * was_im + a_im * was_re + (c_re * drive_im + c_im * drive_re)
        new_re[:, piece(n)] = fresh_re
        new_im[:, piece(n)] = fresh_im
        for copy in write(n):
            copy.start()
        fresh = jnp.concatenate(
            [fresh_re.astype(jnp.bfloat16), fresh_im.astype(jnp.bfloat16)], axis=1
        )
        mixed = lax.dot_general(
            fresh, weights, nt, preferred_element_type=jnp.float32
        ) + skip[:, rows] * u.astype(jnp.float32)
        active[:, rows] = jax.nn.gelu(mixed).astype(jnp.bfloat16)
    for copy in glu:
        copy.wait()
    for name in late:
        small[name].wait()
    acts = active[...]
    value_part = jnp.dot(acts, value[...], preferred_element_type=jnp.float32)
    gate_part = jnp.dot(acts, gate[...], preferred_element_type=jnp.float32)
    branch = value_part * jax.nn.sigmoid(gate_part)
    mid = (residual[...].astype(jnp.float32) + scaled_norm(branch, mix_gain[...])).astype(
        jnp.bfloat16
    )
    resid_mid[...] = mid
    normed[:, head:] = scaled_norm(mid.astype(jnp.float32), in_gain[...]).astype(jnp.bfloat16)
    for n in range(count):
        for copy in write(n):
            copy.wait()


def mixer(
    residual,
    branch_in,
    state_real,
    state_imag,
    decay_rate,
    frequency,
    log_step,
    input_real,
    input_imag,
    output_matrix_real,
    output_matrix_imaginary,
    skip_gain,
    glu_value,
    glu_gate,
    mix_gain,
    moe_in_gain,
    routes,
    route_weights,
):
    group_count, state_count = decay_rate.shape
    inputs = [m.transpose(0, 2, 1).reshape(-1, state_count) for m in (input_real, input_imag)]
    groups = max(1, 128 // input_real.shape[2])
    count = group_count // groups
    vmem = pl.BlockSpec(memory_space=pltpu.VMEM)
    hbm = pl.BlockSpec(memory_space=pltpu.HBM)
    state = state_real.shape
    rows = jax.ShapeDtypeStruct(residual.shape, jnp.bfloat16)
    dma = pltpu.SemaphoreType.DMA
    small = {
        "log_step": log_step[None, :],
        "decay": decay_rate,
        "frequency": frequency,
        "feed": branch_in,
        "in_re": inputs[0],
        "in_im": inputs[1],
        "out_re": output_matrix_real.reshape(-1, state_count),
        "out_im": output_matrix_imaginary.reshape(-1, state_count),
        "skip": skip_gain[None, :],
        "residual": residual,
        "mix_gain": mix_gain[None, :],
        "in_gain": moe_in_gain[None, :],
        "routes": routes.T,
        "route_weights": route_weights.T,
    }
    head = -(-5 * (-(-routes.shape[1] // 8) * 8) // 128) * 128
    wider = (residual.shape[0], residual.shape[1] + head)
    buffers = [(state, jnp.float32)] * 4 + [
        (glu_value.shape, jnp.bfloat16),
        (glu_gate.shape, jnp.bfloat16),
        (branch_in.shape, jnp.bfloat16),
        *[(array.shape, array.dtype) for array in small.values()],
    ]
    used = sum(math.prod(shape) * jnp.dtype(kind).itemsize for shape, kind in buffers)
    return pl.pallas_call(
        functools.partial(mixer_kernel, groups, tuple(small)),
        out_shape=(
            rows,
            jax.ShapeDtypeStruct(wider, jnp.bfloat16),
            jax.ShapeDtypeStruct(state, jnp.float32),
            jax.ShapeDtypeStruct(state, jnp.float32),
        ),
        in_specs=[hbm] * (len(small) + 4),
        out_specs=(vmem, vmem, hbm, hbm),
        scratch_shapes=[pltpu.VMEM(shape, kind) for shape, kind in buffers]
        + [
            dma((len(small),)),
            dma((2, count)),
            dma((2, count)),
            dma((2,)),
        ],
        compiler_params=pltpu.CompilerParams(vmem_limit_bytes=min(VMEM_MOST, used + SPARE)),
        name="mixer",
    )(*in_hbm(*small.values(), state_real, state_imag, glu_value, glu_gate))


def serve_rows(
    residual, branch_in, state_real, state_imag, routes, route_weights, params, capacity
):
    (
        decay_rate,
        frequency,
        log_step,
        input_real,
        input_imag,
        output_matrix_real,
        output_matrix_imaginary,
        skip_gain,
        glu_value,
        glu_gate,
        mix_gain,
        moe_in_gain,
        moe_out_gain,
        expert_gate,
        expert_up,
        expert_down,
        shared_gate,
        shared_up,
        shared_down,
    ) = params
    resid_mid, normed, next_real, next_imag = mixer(
        residual,
        branch_in,
        state_real,
        state_imag,
        decay_rate,
        frequency,
        log_step,
        input_real,
        input_imag,
        output_matrix_real,
        output_matrix_imaginary,
        skip_gain,
        glu_value,
        glu_gate,
        mix_gain,
        moe_in_gain,
        routes,
        route_weights,
    )
    count = lax.axis_size("ep")
    cap = -(-capacity // ROW_TILE) * ROW_TILE
    planes = residual.shape[0] // cap
    width = count // planes
    layer_out = moe_layer(
        normed,
        resid_mid,
        routes.shape[1],
        moe_out_gain,
        (expert_gate[0], expert_up[0], expert_down[0]),
        (shared_gate, shared_up, shared_down),
        planes,
        width,
        cap,
    )
    return (layer_out, next_real, next_imag)


def per_device(
    residual,
    branch_in,
    state_real,
    state_imag,
    decay_rate,
    frequency,
    log_step,
    input_real,
    input_imag,
    output_matrix_real,
    output_matrix_imaginary,
    skip_gain,
    glu_value,
    glu_gate,
    mix_gain,
    moe_in_gain,
    moe_out_gain,
    routes,
    route_weights,
    expert_gate,
    expert_up,
    expert_down,
    shared_gate,
    shared_up,
    shared_down,
):
    params = (
        decay_rate,
        frequency,
        log_step,
        input_real,
        input_imag,
        output_matrix_real,
        output_matrix_imaginary,
        skip_gain,
        glu_value,
        glu_gate,
        mix_gain,
        moe_in_gain,
        moe_out_gain,
        expert_gate,
        expert_up,
        expert_down,
        shared_gate,
        shared_up,
        shared_down,
    )
    seq_dev = residual.shape[0]
    capacity = max(2, 4 * seq_dev * routes.shape[1] // (3 * lax.axis_size("ep")))
    return serve_rows(
        residual, branch_in, state_real, state_imag, routes, route_weights, params, capacity
    )


def solution(mesh):
    return jax.shard_map(
        per_device,
        mesh=mesh,
        in_specs=(
            P("ep", None),
            P("ep", None),
            P("ep", None),
            P("ep", None),
            P(),
            P(),
            P(),
            P(),
            P(),
            P(),
            P(),
            P(),
            P(),
            P(),
            P(),
            P(),
            P(),
            P("ep", None),
            P("ep", None),
            P("ep", None, None),
            P("ep", None, None),
            P("ep", None, None),
            P(),
            P(),
            P(),
        ),
        out_specs=(P("ep", None), P("ep", None), P("ep", None)),
        check_vma=False,
    )
```

```python
import functools
import math

import jax
import jax.numpy as jnp
from jax import lax
from jax.experimental import pallas as pl
from jax.experimental.pallas import tpu as pltpu
from jax.sharding import PartitionSpec as P

norm_eps = 1e-06
ROW_TILE = 16
PIECES = 2
STRIPS = 4
WINDOW = 64
AHEAD = 3
LAG = 1
VMEM_MOST = 60 * 1024 * 1024
SPARE = 8 * 1024 * 1024
MESH = pl.DeviceIdType.MESH


def scaled_norm(row_block, norm_gain):
    return (
        row_block
        * lax.rsqrt(jnp.mean(row_block * row_block, axis=-1, keepdims=True) + norm_eps)
        * norm_gain
    )


def in_hbm(*arrays):
    return [pltpu.with_memory_space_constraint(array, pltpu.HBM) for array in arrays]


def flipped(index, mask):
    out, bit = 0, 1
    while bit <= mask or bit == 1:
        digit = (index // bit) % 2
        out = out + bit * ((digit + 1) % 2 if mask & bit else digit)
        bit *= 2
    return out + (index // bit) * bit


def pick_from(table, z, k):
    value, planes = 0, len(table)
    for row in range(planes):
        away = ((z - row + planes) % planes + planes - 1) // planes
        value = value + table[row][k] * (1 - away)
    return value


def block_order(planes):
    half = max(1, planes // 2)
    order = []
    for z in range(planes):
        others = [b for b in range(planes) if b != z]
        order.append([z] + sorted(others, key=lambda b: (b // half != z // half, abs(b - z), b)))
    return order


def moe_kernel(
    planes,
    width,
    cap,
    top,
    normed,
    resid,
    out_gain_hbm,
    eg_hbm,
    eu_hbm,
    ed_hbm,
    sg_hbm,
    su_hbm,
    sd_hbm,
    out,
    eg,
    eu,
    ed,
    sg,
    su,
    sd,
    out_gain,
    col_rows,
    mix,
    x_send,
    x_recv,
    y_send,
    y_recv,
    part,
    p_send,
    q_recv,
    total,
    load_sem,
    z_s,
    row_r,
    x_s,
    x_r,
    y_s,
    y_r,
    p_s,
    q_r,
):
    me = lax.axis_index("ep")
    z = me // width
    p = me % width
    seq, model = resid.shape
    head = normed.shape[1] - model
    pad = -(-top // 8) * 8
    slots = width * cap
    chunk = model // PIECES
    columns = [slice(i * chunk, (i + 1) * chunk) for i in range(PIECES)]
    pieces = range(PIECES)
    last = planes - 1
    strip = model // STRIPS
    order = block_order(planes)
    upward = [[int(b > r) for b in order[r]] for r in range(planes)]
    behind = [[int(r > 0 if b > r else r < last) for b in order[r]] for r in range(planes)]
    block = [pick_from(order, z, k) for k in range(planes)]

    loads = [
        pltpu.make_async_copy(src, dst, load_sem.at[i])
        for i, (src, dst) in enumerate(
            (
                (sg_hbm, sg),
                (su_hbm, su),
                (sd_hbm, sd),
                (eg_hbm, eg),
                (eu_hbm, eu),
                (ed_hbm, ed),
                (out_gain_hbm, out_gain),
            )
        )
    ]
    for load in (*loads[6:], *loads[:6]):
        load.start()

    barrier = pltpu.get_barrier_semaphore()
    sides = ((z > 0, -1), (z < last, 1)) if planes > 1 else ()
    for there, step in sides:

        @pl.when(there)
        def _():
            pl.semaphore_signal(
                barrier, inc=1, device_id=((z + step) * width + p,), device_id_type=MESH
            )

    for r in range(1, width):
        pl.semaphore_signal(
            barrier, inc=1, device_id=(z * width + flipped(p, r),), device_id_type=MESH
        )

    x_ends, ends = [], []

    def send(src, dst, send_sem, recv_sem, target):
        copy = pltpu.make_async_remote_copy(
            src_ref=src,
            dst_ref=dst,
            send_sem=send_sem,
            recv_sem=recv_sem,
            device_id=(target,),
            device_id_type=MESH,
        )
        copy.start()

    def arrive(buf, sem):
        pltpu.make_async_copy(buf, buf, sem).wait()

    def part_of(buf, k, q, i):
        return buf.at[k, pl.ds(pl.multiple_of(q * cap, cap), cap), columns[i]]

    def table(k):
        rows = normed[:, :head] if k == 0 else col_rows[block[k], :, :head]
        seen = rows.astype(jnp.float32).T
        slot = lax.broadcasted_iota(jnp.int32, (slots, seq), 0)
        expert = (z * width + slot // cap).astype(jnp.float32)
        chosen = jnp.zeros((slots, seq), jnp.float32)
        weight = jnp.zeros((slots, seq), jnp.float32)

        def line(group, j):
            return seen[group * pad + j : group * pad + j + 1, :]

        for j in range(top):
            hit = line(0, j) * 256.0 + line(1, j) == expert
            chosen = jnp.where(hit, 1.0, chosen)
            weight = jnp.where(hit, line(2, j) + line(3, j) + line(4, j), weight)
        earlier = jnp.where(
            lax.broadcasted_iota(jnp.int32, (seq, seq), 0)
            < lax.broadcasted_iota(jnp.int32, (seq, seq), 1),
            1.0,
            0.0,
        ).astype(jnp.bfloat16)
        rank = jnp.dot(chosen.astype(jnp.bfloat16), earlier, preferred_element_type=jnp.float32)
        place = (slot % cap).astype(jnp.float32)
        picks = jnp.where(rank == place, chosen, 0.0)
        spread = (picks * weight).T
        high = spread.astype(jnp.bfloat16)
        mix[k, :seq] = high
        mix[k, seq:] = (spread - high.astype(jnp.float32)).astype(jnp.bfloat16)
        return picks.astype(jnp.bfloat16)

    def gather(k, i, picks):
        span = slice(head + i * chunk, head + (i + 1) * chunk)
        rows = normed[:, span] if k == 0 else col_rows[block[k], :, span]
        x_send[k, :, columns[i]] = jnp.dot(
            picks, rows, preferred_element_type=jnp.float32
        ).astype(jnp.bfloat16)

    def exchange(src, dst, k, i, send_sems, recv_sems, kept):
        for r in range(1, width):
            q = flipped(p, r)
            send(
                part_of(src, k, q, i),
                part_of(dst, k, p, i),
                send_sems.at[k, i],
                recv_sems.at[k, i],
                z * width + q,
            )
        kept.append((src, k, i, send_sems))
        mine = pl.ds(pl.multiple_of(p * cap, cap), cap)
        dst[k, mine, columns[i]] = src[k, mine, columns[i]]

    def others_of(buf, k, i):
        return buf.at[k, slice(cap, width * cap), columns[i]]

    def gathered(dst, k, i, recv_sems):
        if width > 1:
            arrive(others_of(dst, k, i), recv_sems.at[k, i])

    def settle(kept):
        for src, k, i, sems in kept:
            if width > 1:
                arrive(others_of(src, k, i), sems.at[k, i])

    def z_piece(ref, j):
        return ref.at[:, slice(head + j * strip if j else 0, head + (j + 1) * strip)]

    def z_copy(s, f, j):
        source = (z - f + planes) % planes if s == 0 else (z + f) % planes
        buf = col_rows.at[source]
        return pltpu.make_async_remote_copy(
            src_ref=z_piece(buf if f else normed, j),
            dst_ref=z_piece(buf, j),
            send_sem=z_s.at[s, f, j],
            recv_sem=row_r.at[source, j],
            device_id=((z + 1 - 2 * s + planes) % planes * width + p,),
            device_id_type=MESH,
        )

    def moves(s, f):
        return [int(r >= f and r < last) if s == 0 else int(r <= last - f and r > 0) for r in range(planes)]

    def z_sent(s, f, j):
        z_copy(s, f, j).wait_send()

    def z_issue(s, f, j):
        def go():
            before = f * STRIPS + j - WINDOW
            if before >= 0:
                z_sent(s, before // STRIPS, before % STRIPS)
            z_copy(s, f, j).start()

        if any(moves(s, f)):
            pl.when(pick_from([[m] for m in moves(s, f)], z, 0) == 1)(go)

    def z_step(f, j):
        for s in range(2):
            if f:
                source = (z - f + planes) % planes if s == 0 else (z + f) % planes

                @pl.when(z >= f if s == 0 else z <= last - f)
                def _():
                    arrive(z_piece(col_rows.at[source], j), row_r.at[source, j])

            z_issue(s, f, j)

    def z_drain():
        for s in range(2):
            for f in range(planes):
                for j in range(STRIPS):
                    after = (f * STRIPS + j + WINDOW) // STRIPS
                    later = moves(s, after) if after < planes else [0] * planes
                    still = [m * (1 - n) for m, n in zip(moves(s, f), later)]
                    if any(still):
                        pl.when(pick_from([[m] for m in still], z, 0) == 1)(
                            functools.partial(z_sent, s, f, j)
                        )

    def dispatch(k, i, picks):
        gather(k, i, picks)
        exchange(x_send, x_recv, k, i, x_s, x_r, x_ends)

    def hidden(parts, w_gate, w_up):
        gate_part = up_part = 0.0
        for i, rows in enumerate(parts):
            span = columns[i] if len(parts) > 1 else slice(None)
            block_rows = rows()
            gate_part += jnp.dot(block_rows, w_gate[span, :], preferred_element_type=jnp.float32)
            up_part += jnp.dot(block_rows, w_up[span, :], preferred_element_type=jnp.float32)
        return (jax.nn.silu(gate_part) * up_part).astype(jnp.bfloat16)

    def expert(k, ready=()):
        def rows_of(i):
            def rows():
                gathered(x_recv, k, i, x_r)
                return x_recv[k, :, columns[i]]

            return rows

        if k == 0:
            for load in loads[3:6]:
                load.wait()
        mid = hidden([rows_of(i) for i in pieces], eg, eu)
        for i in pieces:
            y_send[k, :, columns[i]] = jnp.dot(
                mid, ed[:, columns[i]], preferred_element_type=jnp.float32
            ).astype(jnp.bfloat16)
            if (k, i) in ready:
                give(k, i)

    def give(k, i):
        exchange(y_send, y_recv, k, i, y_s, y_r, ends)

    def landed(k, i):
        gathered(y_recv, k, i, y_r)

    def weighed(k, i):
        both = jnp.dot(mix[k], y_recv[k, :, columns[i]], preferred_element_type=jnp.float32)
        return both[:seq] + both[seq:]

    def lane(j):
        return slice(j * strip, (j + 1) * strip)

    def strips_of(i):
        return range(i * STRIPS // PIECES, (i + 1) * STRIPS // PIECES)

    def passed_copy(k, j):
        up = pick_from(upward, z, k)
        return pltpu.make_async_remote_copy(
            src_ref=p_send.at[k, :, lane(j)],
            dst_ref=q_recv.at[1 - up, block[k], :, lane(j)],
            send_sem=p_s.at[k, j],
            recv_sem=q_r.at[1 - up, block[k], j],
            device_id=((z - 1 + 2 * up) * width + p,),
            device_id_type=MESH,
        )

    def combine(k, i):
        value = weighed(k, i)
        if k == 0:
            total[:, columns[i]] += value
            return
        part[k, :, columns[i]] = value

        @pl.when(pick_from(behind, z, k) == 0)
        def _():
            for j in strips_of(i):
                p_send[k, :, lane(j)] = part[k, :, lane(j)].astype(jnp.bfloat16)
                passed_copy(k, j).start()

    def merge(k, i):
        up = pick_from(upward, z, k)

        @pl.when(pick_from(behind, z, k) == 1)
        def _():
            for j in strips_of(i):
                landed = q_recv.at[1 - up, block[k], :, lane(j)]
                arrive(landed, q_r.at[1 - up, block[k], j])
                p_send[k, :, lane(j)] = (
                    part[k, :, lane(j)]
                    + q_recv[1 - up, block[k], :, lane(j)].astype(jnp.float32)
                ).astype(jnp.bfloat16)
                passed_copy(k, j).start()

    picks = table(0)
    for i in pieces:
        gather(0, i, picks)

    greeted = [[int(r > 0) + int(r < last)] for r in range(planes)]
    pl.semaphore_wait(barrier, width - 1 + pick_from(greeted, z, 0))
    for j in range(min(WINDOW, STRIPS)):
        z_step(0, j)
    for i in pieces:
        exchange(x_send, x_recv, 0, i, x_s, x_r, x_ends)

    for load in loads[:3]:
        load.wait()
    mid = hidden([lambda: normed[:, head:]], sg, su)
    for i in pieces:
        total[:, columns[i]] = jnp.dot(
            mid, sd[:, columns[i]], preferred_element_type=jnp.float32
        )
    for j in range(min(WINDOW, STRIPS), STRIPS):
        z_step(0, j)
    for k in range(1, planes):
        for i in pieces:
            for j in strips_of(i):
                z_step(k, j)
            if i == 0:
                picks = table(k)
            dispatch(k, i, picks)
        expert(k - 1)
    turns = [(k, i) for k in (*range(last, 0, -1), 0) for i in pieces]
    if planes > 2:
        turns.remove((1, 0))
        turns.insert(0, (1, 0))
        give(1, 0)
    final_own = max((n for n, turn in enumerate(turns) if turn[0] == 1), default=-1)
    first = turns[planes > 2 : AHEAD]
    expert(last, first)
    for turn in first:
        if turn[0] != last:
            give(*turn)
    settle(x_ends)
    done = []
    for n, turn in enumerate(turns):
        landed(*turn)
        if n + AHEAD < len(turns):
            give(*turns[n + AHEAD])
        combine(*turn)
        if turn[0] > 1:
            done.append(turn)
        if turn[0] > 1 and len(done) > LAG:
            merge(*done.pop(0))
        if n == final_own:
            for late in ((1, 0), *done, *((1, i) for i in pieces[1:])):
                merge(*late)
    for side, (there, _) in enumerate(sides):

        @pl.when(there)
        def _():
            for i in pieces:
                for j in strips_of(i):
                    arrive(q_recv.at[side, z, :, lane(j)], q_r.at[side, z, j])
                total[:, columns[i]] += q_recv[side, z, :, columns[i]].astype(jnp.float32)

    loads[6].wait()
    combined = total[...]
    out[...] = (
        resid[...].astype(jnp.float32) + scaled_norm(combined, out_gain[...])
    ).astype(out.dtype)
    settle(ends)
    for k in range(1, planes):
        for j in range(STRIPS):
            passed_copy(k, j).wait_send()
    z_drain()


def moe_layer(
    normed,
    resid_mid,
    top,
    moe_out_gain,
    experts,
    shared_weights,
    planes,
    width,
    cap,
):
    seq_count, model = resid_mid.shape
    half_type = jnp.bfloat16
    vmem = pl.BlockSpec(memory_space=pltpu.VMEM)
    hbm = pl.BlockSpec(memory_space=pltpu.HBM)
    slots = (planes, width * cap, model)
    dense = (planes, seq_count, model)
    dma = pltpu.SemaphoreType.DMA
    weights = (*experts, *shared_weights)
    small = (moe_out_gain[None, :],)
    buffers = [(w.shape, w.dtype) for w in (*weights, *small)] + [
        ((planes, *normed.shape), half_type),
        ((planes, 2 * seq_count, width * cap), half_type),
        (slots, half_type),
        (slots, half_type),
        (slots, half_type),
        (slots, half_type),
        (dense, jnp.float32),
        (dense, half_type),
        ((2, *dense), half_type),
        ((seq_count, model), jnp.float32),
    ]
    used = sum(math.prod(shape) * jnp.dtype(kind).itemsize for shape, kind in buffers)
    return pl.pallas_call(
        functools.partial(moe_kernel, planes, width, cap, top),
        out_shape=jax.ShapeDtypeStruct((seq_count, model), half_type),
        in_specs=[vmem] * 2 + [hbm] * 7,
        out_specs=vmem,
        scratch_shapes=[pltpu.VMEM(shape, kind) for shape, kind in buffers]
        + [
            dma((7,)),
            dma((2, planes, STRIPS)),
            dma((planes, STRIPS)),
            *[dma((planes, PIECES))] * 4,
            dma((planes, STRIPS)),
            dma((2, planes, STRIPS)),
        ],
        compiler_params=pltpu.CompilerParams(
            collective_id=0,
            has_side_effects=True,
            vmem_limit_bytes=min(VMEM_MOST, used + SPARE),
        ),
        name="moe_exchange",
    )(normed, resid_mid, *in_hbm(*small, *weights))


def spread(block, groups, mask):
    return jnp.concatenate([block] * groups, axis=1) * mask


def halves(value):
    high = value.astype(jnp.bfloat16)
    return high, (value - high.astype(jnp.float32)).astype(jnp.bfloat16)


def group_mask(rows, groups, states):
    shape = (rows, groups * states)
    row = lax.broadcasted_iota(jnp.int32, shape, 0) // (rows // groups)
    column = lax.broadcasted_iota(jnp.int32, shape, 1) // states
    return jnp.where(row == column, 1.0, 0.0)


def mixer_kernel(groups, names, *refs):
    count_in = len(names) + 4
    given, rest = refs[:count_in], refs[count_in:]
    state_re, state_im, value_hbm, gate_hbm = given[len(names) :]
    resid_mid, normed, next_re, next_im = rest[:4]
    old_re, old_im, new_re, new_im, value, gate, active = rest[4:11]
    held = dict(zip(names, rest[11 : 11 + len(names)]))
    small_sem, in_sem, out_sem, glu_sem = rest[11 + len(names) :]
    small = {
        name: pltpu.make_async_copy(src, held[name], small_sem.at[i])
        for i, (name, src) in enumerate(zip(names, given))
    }
    decay, frequency, log_step = held["decay"], held["frequency"], held["log_step"]
    in_re, in_im, out_re, out_im = (held[m] for m in ("in_re", "in_im", "out_re", "out_im"))
    residual, feed, skip = held["residual"], held["feed"], held["skip"]
    mix_gain, in_gain = held["mix_gain"], held["in_gain"]
    group_count, states = decay.shape
    chans = in_re.shape[0] // group_count
    lanes = groups * states
    feeds = groups * chans
    count = group_count // groups

    def piece(n):
        return slice(n * lanes, (n + 1) * lanes)

    def read(n):
        return [
            pltpu.make_async_copy(src.at[:, piece(n)], dst.at[:, piece(n)], in_sem.at[k, n])
            for k, (src, dst) in enumerate(((state_re, old_re), (state_im, old_im)))
        ]

    def write(n):
        return [
            pltpu.make_async_copy(src.at[:, piece(n)], dst.at[:, piece(n)], out_sem.at[k, n])
            for k, (src, dst) in enumerate(((new_re, next_re), (new_im, next_im)))
        ]

    glu = [
        pltpu.make_async_copy(value_hbm, value, glu_sem.at[0]),
        pltpu.make_async_copy(gate_hbm, gate, glu_sem.at[1]),
    ]
    late = ("residual", "mix_gain", "in_gain")
    early = ("log_step", "decay", "frequency", "routes", "route_weights")
    for name in names:
        if name not in late:
            small[name].start()
    for n in range(count):
        for copy in read(n):
            copy.start()
    for copy in glu:
        copy.start()
    for name in late:
        small[name].start()

    for name in ("log_step", "decay", "frequency"):
        small[name].wait()
    square = (group_count, group_count)
    diagonal = lax.broadcasted_iota(jnp.int32, square, 0) == lax.broadcasted_iota(
        jnp.int32, square, 1
    )
    step_size = jnp.exp(
        jnp.sum(jnp.where(diagonal, log_step[...], 0.0), axis=1, keepdims=True)
    )
    rate, speed = decay[...], frequency[...]
    magnitude = jnp.exp(-rate * step_size)
    abar_re = magnitude * jnp.cos(speed * step_size)
    abar_im = magnitude * jnp.sin(speed * step_size)
    denominator = rate * rate + speed * speed
    numer_re = abar_re - 1.0
    coef_re = (abar_im * speed - numer_re * rate) / denominator
    coef_im = (-abar_im * rate - numer_re * speed) / denominator

    for name in ("routes", "route_weights"):
        small[name].wait()
    head = normed.shape[1] - resid_mid.shape[1]
    chosen, weight = held["routes"][...], held["route_weights"][...]
    top, seq = chosen.shape
    rest_of = -(-top // 8) * 8 - top
    upper, lower = halves(weight)
    lowest = weight - upper.astype(jnp.float32) - lower.astype(jnp.float32)
    parts = []
    for item in (chosen // 256, chosen % 256, upper, lower, lowest):
        parts += [item.astype(jnp.float32)] + [jnp.zeros((rest_of, seq), jnp.float32)] * (rest_of > 0)
    lines = jnp.concatenate(parts, axis=0)
    lines = jnp.concatenate([lines, jnp.zeros((head - lines.shape[0], seq), jnp.float32)], axis=0)
    normed[:, :head] = lines.T.astype(jnp.bfloat16)

    few = group_mask(groups, groups, states)
    many = group_mask(feeds, groups, states).astype(jnp.bfloat16)
    minus = -many
    nt = (((1,), (1,)), ((), ()))

    for name in names:
        if name not in late and name not in early:
            small[name].wait()
    for n in range(count):
        rows = slice(n * feeds, (n + 1) * feeds)
        some = slice(n * groups, (n + 1) * groups)
        u = feed[:, rows]

        def line(block):
            return jnp.sum(spread(block[some, :], groups, few), axis=0, keepdims=True)

        a_re, a_im, c_re, c_im = line(abar_re), line(abar_im), line(coef_re), line(coef_im)
        drive_re = jnp.dot(
            u, spread(in_re[rows, :], groups, many), preferred_element_type=jnp.float32
        )
        drive_im = jnp.dot(
            u, spread(in_im[rows, :], groups, many), preferred_element_type=jnp.float32
        )
        weights = jnp.concatenate(
            [spread(out_re[rows, :], groups, many), spread(out_im[rows, :], groups, minus)],
            axis=1,
        )
        for copy in read(n):
            copy.wait()
        was_re, was_im = old_re[:, piece(n)], old_im[:, piece(n)]
        fresh_re = a_re * was_re - a_im * was_im + (c_re * drive_re - c_im * drive_im)
        fresh_im = a_re * was_im + a_im * was_re + (c_re * drive_im + c_im * drive_re)
        new_re[:, piece(n)] = fresh_re
        new_im[:, piece(n)] = fresh_im
        for copy in write(n):
            copy.start()
        fresh = jnp.concatenate(
            [fresh_re.astype(jnp.bfloat16), fresh_im.astype(jnp.bfloat16)], axis=1
        )
        mixed = lax.dot_general(
            fresh, weights, nt, preferred_element_type=jnp.float32
        ) + skip[:, rows] * u.astype(jnp.float32)
        active[:, rows] = jax.nn.gelu(mixed).astype(jnp.bfloat16)
    for copy in glu:
        copy.wait()
    for name in late:
        small[name].wait()
    acts = active[...]
    value_part = jnp.dot(acts, value[...], preferred_element_type=jnp.float32)
    gate_part = jnp.dot(acts, gate[...], preferred_element_type=jnp.float32)
    branch = value_part * jax.nn.sigmoid(gate_part)
    mid = (residual[...].astype(jnp.float32) + scaled_norm(branch, mix_gain[...])).astype(
        jnp.bfloat16
    )
    resid_mid[...] = mid
    normed[:, head:] = scaled_norm(mid.astype(jnp.float32), in_gain[...]).astype(jnp.bfloat16)
    for n in range(count):
        for copy in write(n):
            copy.wait()


def mixer(
    residual,
    branch_in,
    state_real,
    state_imag,
    decay_rate,
    frequency,
    log_step,
    input_real,
    input_imag,
    output_matrix_real,
    output_matrix_imaginary,
    skip_gain,
    glu_value,
    glu_gate,
    mix_gain,
    moe_in_gain,
    routes,
    route_weights,
):
    group_count, state_count = decay_rate.shape
    inputs = [m.transpose(0, 2, 1).reshape(-1, state_count) for m in (input_real, input_imag)]
    groups = max(1, 128 // input_real.shape[2])
    count = group_count // groups
    vmem = pl.BlockSpec(memory_space=pltpu.VMEM)
    hbm = pl.BlockSpec(memory_space=pltpu.HBM)
    state = state_real.shape
    rows = jax.ShapeDtypeStruct(residual.shape, jnp.bfloat16)
    dma = pltpu.SemaphoreType.DMA
    small = {
        "log_step": log_step[None, :],
        "decay": decay_rate,
        "frequency": frequency,
        "feed": branch_in,
        "in_re": inputs[0],
        "in_im": inputs[1],
        "out_re": output_matrix_real.reshape(-1, state_count),
        "out_im": output_matrix_imaginary.reshape(-1, state_count),
        "skip": skip_gain[None, :],
        "residual": residual,
        "mix_gain": mix_gain[None, :],
        "in_gain": moe_in_gain[None, :],
        "routes": routes.T,
        "route_weights": route_weights.T,
    }
    head = -(-5 * (-(-routes.shape[1] // 8) * 8) // 128) * 128
    wider = (residual.shape[0], residual.shape[1] + head)
    buffers = [(state, jnp.float32)] * 4 + [
        (glu_value.shape, jnp.bfloat16),
        (glu_gate.shape, jnp.bfloat16),
        (branch_in.shape, jnp.bfloat16),
        *[(array.shape, array.dtype) for array in small.values()],
    ]
    used = sum(math.prod(shape) * jnp.dtype(kind).itemsize for shape, kind in buffers)
    return pl.pallas_call(
        functools.partial(mixer_kernel, groups, tuple(small)),
        out_shape=(
            rows,
            jax.ShapeDtypeStruct(wider, jnp.bfloat16),
            jax.ShapeDtypeStruct(state, jnp.float32),
            jax.ShapeDtypeStruct(state, jnp.float32),
        ),
        in_specs=[hbm] * (len(small) + 4),
        out_specs=(vmem, vmem, hbm, hbm),
        scratch_shapes=[pltpu.VMEM(shape, kind) for shape, kind in buffers]
        + [
            dma((len(small),)),
            dma((2, count)),
            dma((2, count)),
            dma((2,)),
        ],
        compiler_params=pltpu.CompilerParams(vmem_limit_bytes=min(VMEM_MOST, used + SPARE)),
        name="mixer",
    )(*in_hbm(*small.values(), state_real, state_imag, glu_value, glu_gate))


def serve_rows(
    residual, branch_in, state_real, state_imag, routes, route_weights, params, capacity
):
    (
        decay_rate,
        frequency,
        log_step,
        input_real,
        input_imag,
        output_matrix_real,
        output_matrix_imaginary,
        skip_gain,
        glu_value,
        glu_gate,
        mix_gain,
        moe_in_gain,
        moe_out_gain,
        expert_gate,
        expert_up,
        expert_down,
        shared_gate,
        shared_up,
        shared_down,
    ) = params
    resid_mid, normed, next_real, next_imag = mixer(
        residual,
        branch_in,
        state_real,
        state_imag,
        decay_rate,
        frequency,
        log_step,
        input_real,
        input_imag,
        output_matrix_real,
        output_matrix_imaginary,
        skip_gain,
        glu_value,
        glu_gate,
        mix_gain,
        moe_in_gain,
        routes,
        route_weights,
    )
    count = lax.axis_size("ep")
    cap = -(-capacity // ROW_TILE) * ROW_TILE
    planes = residual.shape[0] // cap
    width = count // planes
    layer_out = moe_layer(
        normed,
        resid_mid,
        routes.shape[1],
        moe_out_gain,
        (expert_gate[0], expert_up[0], expert_down[0]),
        (shared_gate, shared_up, shared_down),
        planes,
        width,
        cap,
    )
    return (layer_out, next_real, next_imag)


def per_device(
    residual,
    branch_in,
    state_real,
    state_imag,
    decay_rate,
    frequency,
    log_step,
    input_real,
    input_imag,
    output_matrix_real,
    output_matrix_imaginary,
    skip_gain,
    glu_value,
    glu_gate,
    mix_gain,
    moe_in_gain,
    moe_out_gain,
    routes,
    route_weights,
    expert_gate,
    expert_up,
    expert_down,
    shared_gate,
    shared_up,
    shared_down,
):
    params = (
        decay_rate,
        frequency,
        log_step,
        input_real,
        input_imag,
        output_matrix_real,
        output_matrix_imaginary,
        skip_gain,
        glu_value,
        glu_gate,
        mix_gain,
        moe_in_gain,
        moe_out_gain,
        expert_gate,
        expert_up,
        expert_down,
        shared_gate,
        shared_up,
        shared_down,
    )
    seq_dev = residual.shape[0]
    capacity = max(2, 4 * seq_dev * routes.shape[1] // (3 * lax.axis_size("ep")))
    return serve_rows(
        residual, branch_in, state_real, state_imag, routes, route_weights, params, capacity
    )


def solution(mesh):
    return jax.shard_map(
        per_device,
        mesh=mesh,
        in_specs=(
            P("ep", None),
            P("ep", None),
            P("ep", None),
            P("ep", None),
            P(),
            P(),
            P(),
            P(),
            P(),
            P(),
            P(),
            P(),
            P(),
            P(),
            P(),
            P(),
            P(),
            P("ep", None),
            P("ep", None),
            P("ep", None, None),
            P("ep", None, None),
            P("ep", None, None),
            P(),
            P(),
            P(),
        ),
        out_specs=(P("ep", None), P("ep", None), P("ep", None)),
        check_vma=False,
    )
```
